256 devices in a mesh: grp: 2 (over z), ep: 16 (over y, core), tp: 8 (over x).
Axes of the slice: x: 8, y: 8, z: 2, core: 2. Of those that a mesh axis runs over, the one named last changes fastest.
The devices are a block of a 8x8x16 slice.
Arguments:
- tokens: bfloat16 [32768, 1024], P(('grp', 'ep', 'tp')), parts along dimension 0, may hold values from -6 to 6
- norm_gain: float32 [1024], replicated, may hold values from 0.1 to 1.9
- gate_weight: bfloat16 [16, 1024, 3584], P('ep', None, 'tp'), may hold values from -0.1875 to 0.1875
- up_weight: bfloat16 [16, 1024, 3584], P('ep', None, 'tp'), may hold values from -0.1875 to 0.1875
- down_weight: bfloat16 [16, 3584, 1024], P('ep', 'tp'), may hold values from -0.09375 to 0.09375
- expert_ids: int32 [32768, 2], P(('grp', 'ep')), parts along dimension 0, may hold values from 0 to 15, all different within a row; in each aligned block of 128 rows (0 to 127, 128 to 255, ...) at most 20 rows name the same one
- route_weight: float32 [32768, 2], P(('grp', 'ep')), parts along dimension 0, may hold values from 0.2 to 1
Outputs:
- mixed: bfloat16 [32768, 1024], P(('grp', 'ep', 'tp')), parts along dimension 0
The draws below stay inside these ranges and needn't reach their ends.
There are 2 independent parts, one for each index of `grp`. The reference program is written for one: setup_inputs(seed, part) draws one part's arguments, and reference() takes and returns one part's arrays. A program takes and returns all parts, laid end to end along the dimension named above; an argument that names none is the same for every part. Nothing has to cross between parts.
Inputs may be any that keep to these rules, and one draw needn't show every extreme that they name: `expert_ids`: A token's 2 experts differ. In the rows of one device (128 tokens, aligned blocks) no expert is named more than 20 times, and in every draw some expert is named exactly 20 times in some device's rows.
All inputs are finite; a program needn't handle non-finite values.
Results may differ from the reference program's by a relative error of at most 0.015.
Values may be sent and summed in bfloat16 or wider, within the bound.
No kernel may reach another device: no remote copies, remote signals or barrier semaphores. Data moves between devices by JAX's collectives and lax.ppermute only.
A program may use at most 64 MiB of HBM per device.

```python
import math
import jax
import jax.numpy as jnp
import numpy as np
from jax import lax

D = 1024
FF = 3584
TOP_K = 2
TOK_DEV = 128
EXPERTS = 16
TOKENS = 16384
MOST = 20
N_EP = 16
N_TP = 8


def shard_levels(rng, shape, split, least, high):
    gain = 1.0
    for position, shards_of in split:
        steps = jax.random.uniform(jax.random.fold_in(jax.random.fold_in(rng, 6), position), (shards_of,), jnp.float32, least / len(split), high / len(split))
        gain = gain * jnp.repeat(jnp.exp(steps), shape[position] // shards_of).reshape((-1,) + (1,) * (len(shape) - 1 - position))
    return gain


def deal_out(rng, own, number, rows, count, top, most, skew):
    sequence = jax.random.permutation(rng, count)
    crowded, usual = portions_of(count, rows * top, most, skew, True), portions_of(count, rows * top, most, skew, False)
    places = jnp.arange(count)

    def named(lengths, turn):
        used = int((lengths > 0).sum())
        fixed = max(1, used // 4)
        moved = fixed + (places - fixed + turn * (used - fixed)) % max(1, count - fixed)
        return jnp.zeros((count,), jnp.int32).at[sequence[jnp.where(places < fixed, places, moved)]].set(jnp.asarray(lengths, jnp.int32))

    lengths = jnp.where(number % 4 == 0, named(crowded, number // 4), named(usual, number - number // 4 - 1))
    mixed = jax.random.permutation(jax.random.fold_in(own, 3), count)
    giver, sink = mixed[0:count // 2 * 2:2], mixed[1:count // 2 * 2:2]
    slack = jnp.minimum(lengths[giver] - 1, most - lengths[sink]) // 2
    slack = jnp.where((giver == sequence[0]) | (sink == sequence[0]) | (lengths[sink] == 0), 0, jnp.maximum(slack, 0))
    moved = jax.random.randint(jax.random.fold_in(own, 4), (count // 2,), 0, 1 << 20) % (slack + 1)
    lengths = lengths.at[giver].add(-moved).at[sink].add(moved)
    items = jnp.searchsorted(jnp.cumsum(lengths), jnp.arange(rows * top), side="right").astype(jnp.int32)
    table = items.reshape(top, rows).T
    table = table[jax.random.permutation(jax.random.fold_in(own, 1), rows)]
    turn = jax.random.randint(jax.random.fold_in(own, 2), (rows, 1), 0, top)
    return jnp.take_along_axis(table, (jnp.arange(top)[None, :] + turn) % top, axis=1)


def portions_of(count, total, most, lean, full):
    weights = [(1 << 20) // math.isqrt(grade ** lean) + 1 for grade in range(1, count + 1)]
    largest = most if full else min(most, max(-(-total // count), total * weights[0] // sum(weights)))
    least = 1 if total - largest >= count - 1 else 0
    given, rest = [largest] + [least] * (count - 1), total - largest - least * (count - 1)
    while rest > 0:
        candidates = [i for i in range(1, count) if given[i] < largest] or [i for i in range(1, count) if given[i] < most]
        pool, budget = sum([weights[i] for i in candidates]), rest
        for i in candidates:
            more = min(most - given[i], max(1, budget * weights[i] // pool), rest)
            given[i] = given[i] + more
            rest = rest - more
    return np.array(given)


def centred(rng, extent, spread, bound, shards=(), held_as=jnp.bfloat16):
    result = jax.random.normal(rng, extent, jnp.float32) * spread
    if len(shards) > 0:
        result = shard_levels(rng, extent, shards, -0.22, 0.18) * result
    return jnp.clip(result, min=-bound, max=bound).astype(held_as)


def setup_inputs(seed: int = 0, part: int = 0) -> dict:
    streams_of = jax.random.split(jax.random.key(seed), 8)
    own_keys = jax.random.split(jax.random.fold_in(streams_of[7], part), 8)
    tokens = centred(own_keys[0], (TOKENS, D), 1.0, 6.0, ((0, 128),))
    norm_gain = jnp.clip(1.0 + 0.18 * jax.random.normal(streams_of[1], (D,), jnp.float32), 0.1, 1.9)
    gate_weight = centred(streams_of[2], (EXPERTS, D, FF), D ** -0.5, 0.1875, ((0, 16), (2, 8)))
    up_weight = centred(streams_of[3], (EXPERTS, D, FF), D ** -0.5, 0.1875, ((0, 16), (2, 8)))
    down_weight = centred(streams_of[4], (EXPERTS, FF, D), FF ** -0.5, 0.09375, ((0, 16), (1, 8)))
    expert_ids_keys = jax.random.split(jax.random.fold_in(own_keys[5], 1), TOKENS // TOK_DEV)
    expert_ids_turns = jax.random.permutation(jax.random.fold_in(own_keys[5], 3), TOKENS // TOK_DEV)
    expert_ids = jax.vmap(lambda own, number: deal_out(jax.random.fold_in(own_keys[5], 2), own, number, TOK_DEV, EXPERTS, TOP_K, MOST, 2))(expert_ids_keys, expert_ids_turns).reshape((TOKENS, TOP_K))
    route_weight = jnp.clip(0.2 + 0.8 * jax.random.uniform(own_keys[6], (TOKENS, TOP_K), jnp.float32) ** shard_levels(own_keys[6], (TOKENS, TOP_K), ((0, 16),), -0.2, 0.2), 0.2, 1.0)
    return dict(tokens=tokens, norm_gain=norm_gain, gate_weight=gate_weight, up_weight=up_weight, down_weight=down_weight, expert_ids=expert_ids, route_weight=route_weight)


def norm_rows(tokens, norm_gain):
    values = tokens.astype(jnp.float32)
    scaled = values * lax.rsqrt(lax.optimization_barrier(jnp.mean(values * values, axis=-1, keepdims=True)) + 1e-06)
    return (scaled * norm_gain.astype(jnp.float32)).astype(jnp.bfloat16)

def reference(tokens, norm_gain, gate_weight, up_weight, down_weight, expert_ids, route_weight):
    normed = norm_rows(tokens, norm_gain)
    devices_all = N_EP * N_TP
    cap_rows = devices_all * MOST
    flat_ids = expert_ids.astype(jnp.int32).reshape(devices_all, TOK_DEV * TOP_K)
    onehot = (flat_ids[:, :, None] == jnp.arange(EXPERTS, dtype=jnp.int32)[None, None, :]).astype(jnp.int32)
    before = jnp.cumsum(onehot, axis=1) - onehot
    slots = lax.optimization_barrier(jnp.sum(before * onehot, axis=-1))
    owner = jnp.arange(devices_all, dtype=jnp.int32)[:, None]
    row_index = (flat_ids * cap_rows + owner * MOST + slots).reshape(-1).astype(jnp.int32)
    repeated = jnp.repeat(normed, TOP_K, axis=0)
    buffer = jnp.zeros((EXPERTS * cap_rows, D), jnp.bfloat16).at[row_index].set(repeated)
    buffer = buffer.reshape(EXPERTS, cap_rows, D)
    block = FF // N_TP

    def shard_step(total, shard):
        start = (shard * block).astype(jnp.int32)

        def one_expert(items):
            rows, w_gate, w_up, w_down = items
            gate_part = lax.dynamic_slice_in_dim(w_gate, start, block, 1)
            up_part = lax.dynamic_slice_in_dim(w_up, start, block, 1)
            down_part = lax.dynamic_slice_in_dim(w_down, start, block, 0)
            gate = jnp.dot(rows, gate_part, preferred_element_type=jnp.float32)
            upper = jnp.dot(rows, up_part, preferred_element_type=jnp.float32)
            hidden = (jax.nn.silu(gate) * upper).astype(jnp.bfloat16)
            return jnp.dot(hidden, down_part, preferred_element_type=jnp.float32).astype(jnp.bfloat16)
        pieces = lax.map(one_expert, (buffer, gate_weight, up_weight, down_weight))
        picked = pieces.reshape(EXPERTS * cap_rows, D)[row_index].reshape(TOKENS, TOP_K, D)
        return (total + picked.astype(jnp.float32), None)
    total, _ = lax.scan(shard_step, jnp.zeros((TOKENS, TOP_K, D), jnp.float32), jnp.arange(N_TP, dtype=jnp.int32))
    piece = lax.optimization_barrier(total.astype(jnp.bfloat16))
    weighted = lax.optimization_barrier(jnp.sum(piece.astype(jnp.float32) * route_weight.astype(jnp.float32)[:, :, None], axis=1))
    return weighted.astype(jnp.bfloat16)
```

```python
import functools

import jax
import jax.numpy as jnp
from jax import lax
from jax.experimental import pallas as pl
from jax.experimental.pallas import tpu as pltpu
from jax.sharding import PartitionSpec as P

TOP_K = 2
CORES = 2
F32 = jnp.float32
BF16 = jnp.bfloat16


def dispatch_kernel(place, tok_a, tok_b, gain, ids_a, ids_b, wts_a, wts_b, *outs, chips, slots):
    blocks, mix_hi, mix_lo = outs[:chips], outs[chips], outs[chips + 1]
    tp, chip, core = place[0], place[1], place[2]
    rows = tok_a.shape[0]
    both = CORES * rows
    total = chips * slots

    def normed(tok):
        values = tok[...].astype(F32)
        scaled = values * lax.rsqrt(jnp.mean(values * values, axis=-1, keepdims=True) + 1e-06)
        return (scaled * gain[...]).astype(BF16)

    def columns(ids, wts):
        start = pl.multiple_of(tp * rows, rows)
        meta = jnp.concatenate(
            [ids[:, pl.ds(start, rows)].astype(F32), wts[:, pl.ds(start, rows)]]
            + [jnp.zeros((8 - 2 * TOP_K, rows), F32)],
            axis=0,
        )
        return meta.T

    meta = jnp.concatenate([columns(ids_a, wts_a), columns(ids_b, wts_b)], axis=0)
    experts = meta[:, 0:TOP_K].astype(jnp.int32)
    distance = jnp.where(experts % CORES == core, (experts // CORES - chip + chips) % chips, -1)
    lane = lax.broadcasted_iota(jnp.int32, (both, 128), 1)
    hot = [lane == distance[:, k : k + 1] for k in range(TOP_K)]
    named = (hot[0] | hot[1]).astype(F32).astype(BF16)
    earlier = lax.broadcasted_iota(jnp.int32, (both, both), 1) < lax.broadcasted_iota(
        jnp.int32, (both, both), 0
    )
    rank = jnp.dot(earlier.astype(F32).astype(BF16), named, preferred_element_type=F32)
    row = lax.broadcasted_iota(jnp.int32, (both, total), 1)
    here = []
    for k in range(TOP_K):
        slot = jnp.sum(jnp.where(hot[k], rank, 0.0), axis=1, keepdims=True).astype(jnp.int32)
        at = jnp.where(distance[:, k : k + 1] < 0, -1, distance[:, k : k + 1] * slots + slot)
        here.append(row == at)
    send = (here[0] | here[1]).astype(F32).astype(BF16)
    values = jnp.concatenate([normed(tok_a), normed(tok_b)], axis=0)
    packed = lax.dot_general(
        send, values, (((0,), (0,)), ((), ())), preferred_element_type=F32
    )
    for d in range(chips):
        blocks[d][...] = packed[d * slots : (d + 1) * slots].astype(BF16)
    mix = jnp.where(here[0], meta[:, TOP_K : TOP_K + 1], 0.0) + jnp.where(
        here[1], meta[:, TOP_K + 1 : TOP_K + 2], 0.0
    )
    high = mix.astype(BF16)
    mix_hi[...] = high
    mix_lo[...] = (mix - high.astype(F32)).astype(BF16)


def combine_kernel(mix_hi, mix_lo, *refs):
    blocks, own, other = refs[:-2], refs[-2], refs[-1]
    pieces = jnp.concatenate([b[...].astype(F32) for b in blocks], axis=0).astype(BF16)
    total = jnp.dot(mix_hi[...], pieces, preferred_element_type=F32)
    total = total + jnp.dot(mix_lo[...], pieces, preferred_element_type=F32)
    half = total.shape[0] // CORES
    own[...] = total[:half]
    other[...] = total[half:].astype(BF16)


def ffn_kernel(gate_w, up_w, down_w, *refs):
    count = len(refs) // 2
    contract = (((1,), (1,)), ((), ()))
    for source, out in zip(refs[:count], refs[count:]):
        rows = source[...]
        gate = lax.dot_general(rows, gate_w[...], contract, preferred_element_type=F32)
        upper = lax.dot_general(rows, up_w[...], contract, preferred_element_type=F32)
        hidden = (gate / (1.0 + jnp.exp(-gate)) * upper).astype(BF16)
        out[...] = jnp.dot(hidden, down_w[...], preferred_element_type=F32).astype(BF16)


VMEM = pl.BlockSpec(memory_space=pltpu.VMEM)
PARAMS = pltpu.CompilerParams(vmem_limit_bytes=24 * 1024 * 1024)


def body(tokens, norm_gain, gate_weight, up_weight, down_weight, expert_ids, route_weight):
    tok_rows, width = tokens.shape
    n_tp = lax.axis_size("tp")
    n_ep = lax.axis_size("ep")
    chips = n_ep // CORES
    most = max(2, tok_rows * TOP_K * 5 // (4 * n_ep))
    slots = CORES * most
    ep = lax.axis_index("ep")
    place = jnp.stack([lax.axis_index("tp"), ep // CORES, ep % CORES]).astype(jnp.int32)

    def swap(values):
        return lax.ppermute(values, "ep", [(i, i ^ 1) for i in range(n_ep)])

    def over_chips(values, d):
        pairs = [(i, (i + CORES * d) % n_ep) for i in range(n_ep)]
        return lax.ppermute(values, "ep", pairs)

    def over_tp(values, step):
        return lax.ppermute(values, "tp", [(i, (i + step) % n_tp) for i in range(n_tp)])

    tok_b = swap(tokens)
    ids_b = swap(expert_ids)
    wts_b = swap(route_weight)
    out_types = [jax.ShapeDtypeStruct((slots, width), BF16)] * chips
    out_types += [jax.ShapeDtypeStruct((CORES * tok_rows, chips * slots), BF16)] * 2
    *blocks, mix_hi, mix_lo = pl.pallas_call(
        functools.partial(dispatch_kernel, chips=chips, slots=slots),
        in_specs=[pl.BlockSpec(memory_space=pltpu.SMEM)] + [VMEM] * 7,
        out_specs=[VMEM] * (chips + 2),
        out_shape=out_types,
        compiler_params=PARAMS,
        name="dispatch",
    )(place, tokens, tok_b, norm_gain[None], expert_ids.T, ids_b.T, route_weight.T, wts_b.T)

    near = [0, 1, chips - 1, 2]
    far = [d for d in range(chips) if d not in near]
    gate_t = gate_weight[0].T
    up_t = up_weight[0].T
    down = down_weight[0]

    def ffn(*sources):
        return pl.pallas_call(
            ffn_kernel,
            in_specs=[VMEM] * (3 + len(sources)),
            out_specs=[VMEM] * len(sources),
            out_shape=[jax.ShapeDtypeStruct(s.shape, BF16) for s in sources],
            compiler_params=PARAMS,
            name="ffn",
        )(gate_t, up_t, down, *sources)

    half_way = n_tp // 2
    returned = [None] * chips
    for group, way in ((near, 1), (far, -1)):
        chunk = jnp.concatenate([over_chips(blocks[d], d) if d else blocks[d] for d in group], axis=0)
        fore = [chunk]
        back = [chunk]
        for step in range(half_way):
            fore.append(over_tp(fore[-1], way))
            if step < n_tp - 1 - half_way:
                back.append(over_tp(back[-1], -way))
        part_fore = [None] * (half_way + 1)
        part_back = [None] * half_way
        for step in range(1, half_way + 1):
            if step < half_way:
                part_fore[step], part_back[step] = ffn(fore[step], back[step])
            else:
                (part_fore[step],) = ffn(fore[step])
        (mine,) = ffn(chunk)
        total_fore = part_fore[half_way]
        for step in range(half_way - 1, 0, -1):
            got = over_tp(total_fore, -way)
            total_fore = (got.astype(F32) + part_fore[step].astype(F32)).astype(BF16)
        total_back = part_back[half_way - 1]
        for step in range(half_way - 2, 0, -1):
            got = over_tp(total_back, way)
            total_back = (got.astype(F32) + part_back[step].astype(F32)).astype(BF16)
        total_fore = over_tp(total_fore, -way)
        total_back = over_tp(total_back, way)
        pieces = (
            mine.astype(F32) + total_fore.astype(F32) + total_back.astype(F32)
        ).astype(BF16)
        for j, d in enumerate(group):
            piece = pieces[j * slots : (j + 1) * slots]
            returned[d] = over_chips(piece, -d) if d else piece

    own, other = pl.pallas_call(
        combine_kernel,
        in_specs=[VMEM] * (2 + chips),
        out_specs=[VMEM] * 2,
        out_shape=[
            jax.ShapeDtypeStruct((tok_rows, width), F32),
            jax.ShapeDtypeStruct((tok_rows, width), BF16),
        ],
        compiler_params=PARAMS,
        name="combine",
    )(mix_hi, mix_lo, *returned)
    return (own + swap(other).astype(F32)).astype(BF16)


def solution(mesh):
    placed = (
        P(("grp", "ep", "tp"), None),
        P(),
        P("ep", None, "tp"),
        P("ep", None, "tp"),
        P("ep", "tp", None),
        P(("grp", "ep"), None),
        P(("grp", "ep"), None),
    )
    return jax.shard_map(
        body, mesh=mesh, in_specs=placed, out_specs=P(("grp", "ep", "tp"), None), check_vma=False
    )
```

```python
import functools

import jax
import jax.numpy as jnp
from jax import lax
from jax.experimental import pallas as pl
from jax.experimental.pallas import tpu as pltpu
from jax.sharding import PartitionSpec as P


TOP_K = 2
CORES = 2
F32 = jnp.float32
BF16 = jnp.bfloat16


def norm_kernel(tok, gain, out):
    values = tok[...].astype(F32)
    scaled = values * lax.rsqrt(jnp.mean(values * values, axis=-1, keepdims=True) + 1e-06)
    out[...] = (scaled * gain[...]).astype(BF16)


def dispatch_kernel(place, norm_a, tok_b, gain, ids_a, ids_b, wts_a, wts_b, *refs, chips, slots):
    blocks, mix_hi, mix_lo, values = refs[:chips], refs[chips], refs[chips + 1], refs[chips + 2]
    tp, chip, core = place[0], place[1], place[2]
    rows = norm_a.shape[0]
    both = CORES * rows
    total = chips * slots
    values[:rows] = norm_a[...]
    norm_kernel(tok_b, gain, values.at[rows:])

    def columns(ids, wts):
        start = pl.multiple_of(tp * rows, rows)
        meta = jnp.concatenate(
            [ids[:, pl.ds(start, rows)].astype(F32), wts[:, pl.ds(start, rows)]]
            + [jnp.zeros((8 - 2 * TOP_K, rows), F32)],
            axis=0,
        )
        return meta.T

    meta = jnp.concatenate([columns(ids_a, wts_a), columns(ids_b, wts_b)], axis=0)
    experts = meta[:, 0:TOP_K].astype(jnp.int32)
    distance = jnp.where(experts % CORES == core, (experts // CORES - chip + chips) % chips, -1)
    lane = lax.broadcasted_iota(jnp.int32, (both, 128), 1)
    hot = [lane == distance[:, k : k + 1] for k in range(TOP_K)]
    named = (hot[0] | hot[1]).astype(F32).astype(BF16)
    earlier = lax.broadcasted_iota(jnp.int32, (both, both), 1) < lax.broadcasted_iota(
        jnp.int32, (both, both), 0
    )
    rank = jnp.dot(earlier.astype(F32).astype(BF16), named, preferred_element_type=F32)
    row = lax.broadcasted_iota(jnp.int32, (both, total), 1)
    here = []
    for k in range(TOP_K):
        slot = jnp.sum(jnp.where(hot[k], rank, 0.0), axis=1, keepdims=True).astype(jnp.int32)
        at = jnp.where(distance[:, k : k + 1] < 0, -1, distance[:, k : k + 1] * slots + slot)
        here.append(row == at)
    send = (here[0] | here[1]).astype(F32).astype(BF16)
    packed = lax.dot_general(
        send, values[...], (((0,), (0,)), ((), ())), preferred_element_type=F32
    )
    for d in range(chips):
        blocks[d][...] = packed[d * slots : (d + 1) * slots].astype(BF16)
    mix = jnp.where(here[0], meta[:, TOP_K : TOP_K + 1], 0.0) + jnp.where(
        here[1], meta[:, TOP_K + 1 : TOP_K + 2], 0.0
    )
    high = mix.astype(BF16)
    mix_hi[...] = high
    mix_lo[...] = (mix - high.astype(F32)).astype(BF16)


def combine_kernel(mix_hi, mix_lo, *refs):
    blocks, own, other = refs[:-2], refs[-2], refs[-1]
    pieces = jnp.concatenate([b[...].astype(F32) for b in blocks], axis=0).astype(BF16)
    total = jnp.dot(mix_hi[...], pieces, preferred_element_type=F32)
    total = total + jnp.dot(mix_lo[...], pieces, preferred_element_type=F32)
    half = total.shape[0] // CORES
    own[...] = total[:half]
    other[...] = total[half:].astype(BF16)


def ffn_kernel(gate_w, up_w, down_w, *refs):
    count = (len(refs) - 2) // 2
    gate_sum, up_sum = refs[-2:]
    contract = (((1,), (1,)), ((), ()))
    width = gate_w.shape[1]
    tile = min(256, width)
    for source, out in zip(refs[:count], refs[count : 2 * count]):

        def features(i, source=source):
            at = pl.ds(pl.multiple_of(i * tile, tile), tile)
            rows = source[:, at]
            gate = lax.dot_general(rows, gate_w[:, at], contract, preferred_element_type=F32)
            upper = lax.dot_general(rows, up_w[:, at], contract, preferred_element_type=F32)
            return gate, upper

        gate_sum[...], up_sum[...] = features(0)

        @pl.loop(1, width // tile)
        def _(i, features=features):
            gate, upper = features(i)
            gate_sum[...] += gate
            up_sum[...] += upper

        gate = gate_sum[...]
        hidden = (gate / (1.0 + jnp.exp(-gate)) * up_sum[...]).astype(BF16)

        @pl.loop(0, width // tile)
        def _(i, out=out, hidden=hidden):
            at = pl.ds(pl.multiple_of(i * tile, tile), tile)
            out[:, at] = jnp.dot(hidden, down_w[:, at], preferred_element_type=F32).astype(BF16)


VMEM = pl.BlockSpec(memory_space=pltpu.VMEM)
PARAMS = pltpu.CompilerParams(vmem_limit_bytes=24 * 1024 * 1024)


def chunks_of(chips):
    near = sorted({0, 1 % chips, chips - 1})
    return near, sorted(set(range(chips)) - set(near), key=lambda d: min(d, chips - d))


def body(tokens, norm_gain, gate_weight, up_weight, down_weight, expert_ids, route_weight):
    tok_rows, width = tokens.shape
    n_tp = lax.axis_size("tp")
    n_ep = lax.axis_size("ep")
    chips = n_ep // CORES
    most = max(2, tok_rows * TOP_K * 5 // (4 * n_ep))
    slots = CORES * most
    ep = lax.axis_index("ep")
    place = jnp.stack([lax.axis_index("tp"), ep // CORES, ep % CORES]).astype(jnp.int32)

    def swap(values):
        return lax.ppermute(values, "ep", [(i, i ^ 1) for i in range(n_ep)])

    def over_chips(values, d):
        pairs = [(i, (i + CORES * d) % n_ep) for i in range(n_ep)]
        return lax.ppermute(values, "ep", pairs)

    def over_tp(values, step):
        return lax.ppermute(values, "tp", [(i, (i + step) % n_tp) for i in range(n_tp)])

    tok_b = swap(tokens)
    ids_b = swap(expert_ids)
    wts_b = swap(route_weight)
    norm_a = pl.pallas_call(
        norm_kernel,
        in_specs=[VMEM] * 2,
        out_specs=VMEM,
        out_shape=jax.ShapeDtypeStruct(tokens.shape, BF16),
        compiler_params=PARAMS,
        name="norm_own",
    )(tokens, norm_gain[None])
    out_types = [jax.ShapeDtypeStruct((slots, width), BF16)] * chips
    out_types += [jax.ShapeDtypeStruct((CORES * tok_rows, chips * slots), BF16)] * 2
    *blocks, mix_hi, mix_lo = pl.pallas_call(
        functools.partial(dispatch_kernel, chips=chips, slots=slots),
        in_specs=[pl.BlockSpec(memory_space=pltpu.SMEM)] + [VMEM] * 7,
        out_specs=[VMEM] * (chips + 2),
        out_shape=out_types,
        scratch_shapes=[pltpu.VMEM((CORES * tok_rows, width), BF16)],
        compiler_params=PARAMS,
        name="dispatch",
    )(place, norm_a, tok_b, norm_gain[None], expert_ids.T, ids_b.T, route_weight.T, wts_b.T)

    gate_t = gate_weight[0].T
    up_t = up_weight[0].T
    down = down_weight[0]

    def ffn(*sources):
        sums = pltpu.VMEM((sources[0].shape[0], gate_t.shape[0]), F32)
        return pl.pallas_call(
            ffn_kernel,
            in_specs=[VMEM] * (3 + len(sources)),
            out_specs=[VMEM] * len(sources),
            out_shape=[jax.ShapeDtypeStruct(s.shape, BF16) for s in sources],
            scratch_shapes=[sums, sums],
            compiler_params=PARAMS,
            name="ffn",
        )(gate_t, up_t, down, *sources)

    def add(got, part):
        return (got.astype(F32) + part.astype(F32)).astype(BF16)

    half = n_tp // 2
    returned = [None] * chips
    for group, way in zip(chunks_of(chips), (1, -1)):
        chunk = jnp.concatenate(
            [over_chips(blocks[d], d) if d else blocks[d] for d in group], axis=0
        )
        fore, back = [chunk], [chunk]
        for s in range(1, half + 1):
            fore.append(over_tp(fore[-1], way))
            if s < half:
                back.append(over_tp(back[-1], -way))
        (mine,) = ffn(chunk)
        parts = [None] + [ffn(fore[s], back[s]) for s in range(1, half)]
        (total_fore,) = ffn(fore[half])
        total_back = parts[half - 1][1]
        for h in range(1, half + 1):
            got = over_tp(total_fore, -way)
            total_fore = add(got, parts[half - h][0]) if h < half else got
        for h in range(1, half):
            got = over_tp(total_back, way)
            total_back = add(got, parts[half - 1 - h][1]) if h < half - 1 else got
        pieces = (
            mine.astype(F32) + total_fore.astype(F32) + total_back.astype(F32)
        ).astype(BF16)
        for j, d in enumerate(group):
            piece = pieces[j * slots : (j + 1) * slots]
            returned[d] = over_chips(piece, -d) if d else piece

    own, other = pl.pallas_call(
        combine_kernel,
        in_specs=[VMEM] * (2 + chips),
        out_specs=[VMEM] * 2,
        out_shape=[
            jax.ShapeDtypeStruct((tok_rows, width), F32),
            jax.ShapeDtypeStruct((tok_rows, width), BF16),
        ],
        compiler_params=PARAMS,
        name="combine",
    )(mix_hi, mix_lo, *returned)
    return (own + swap(other).astype(F32)).astype(BF16)


def solution(mesh):
    placed = (
        P(("grp", "ep", "tp"), None),
        P(),
        P("ep", None, "tp"),
        P("ep", None, "tp"),
        P("ep", "tp", None),
        P(("grp", "ep"), None),
        P(("grp", "ep"), None),
    )
    return jax.shard_map(
        body, mesh=mesh, in_specs=placed, out_specs=P(("grp", "ep", "tp"), None), check_vma=False
    )
```

```python
import functools

import jax
import jax.numpy as jnp
from jax import lax
from jax.experimental import pallas as pl
from jax.experimental.pallas import tpu as pltpu
from jax.sharding import PartitionSpec as P


TOP_K = 2
CORES = 2
HOP = 2
F32 = jnp.float32
BF16 = jnp.bfloat16
VMEM = pl.BlockSpec(memory_space=pltpu.VMEM)
PARAMS = pltpu.CompilerParams(vmem_limit_bytes=24 * 1024 * 1024)


def norm_kernel(tok, gain, out):
    values = tok[...].astype(F32)
    scaled = values * lax.rsqrt(jnp.mean(values * values, axis=-1, keepdims=True) + 1e-06)
    out[...] = (scaled * gain[...]).astype(BF16)


def dispatch_kernel(place, norm_a, tok_b, gain, meta_a, meta_b, *refs, chips, slots):
    blocks, mix_hi, mix_lo, values = refs[:chips], refs[chips], refs[chips + 1], refs[chips + 2]
    chip, core = place[0], place[1]
    rows = norm_a.shape[0]
    both = CORES * rows
    total = chips * slots
    values[:rows] = norm_a[...]
    norm_kernel(tok_b, gain, values.at[rows:])
    meta = jnp.concatenate([meta_a[...].T, meta_b[...].T], axis=0)
    experts = meta[:, 0:TOP_K].astype(jnp.int32)
    distance = jnp.where(experts % CORES == core, (experts // CORES - chip + chips) % chips, -1)
    lane = lax.broadcasted_iota(jnp.int32, (both, 128), 1)
    hot = [lane == distance[:, k : k + 1] for k in range(TOP_K)]
    named = (hot[0] | hot[1]).astype(F32).astype(BF16)
    earlier = lax.broadcasted_iota(jnp.int32, (both, both), 1) < lax.broadcasted_iota(
        jnp.int32, (both, both), 0
    )
    rank = jnp.dot(earlier.astype(F32).astype(BF16), named, preferred_element_type=F32)
    row = lax.broadcasted_iota(jnp.int32, (both, total), 1)
    here = []
    for k in range(TOP_K):
        slot = jnp.sum(jnp.where(hot[k], rank, 0.0), axis=1, keepdims=True).astype(jnp.int32)
        at = jnp.where(distance[:, k : k + 1] < 0, -1, distance[:, k : k + 1] * slots + slot)
        here.append(row == at)
    send = (here[0] | here[1]).astype(F32).astype(BF16)
    packed = lax.dot_general(
        send, values[...], (((0,), (0,)), ((), ())), preferred_element_type=F32
    )
    for d in range(chips):
        blocks[d][...] = packed[d * slots : (d + 1) * slots].astype(BF16)
    mix = jnp.where(here[0], meta[:, TOP_K : TOP_K + 1], 0.0) + jnp.where(
        here[1], meta[:, TOP_K + 1 : TOP_K + 2], 0.0
    )
    high = mix.astype(BF16)
    mix_hi[...] = high
    mix_lo[...] = (mix - high.astype(F32)).astype(BF16)


def combine_kernel(mix_hi, mix_lo, *refs):
    blocks, own, other = refs[:-2], refs[-2], refs[-1]
    pieces = jnp.concatenate([b[...].astype(F32) for b in blocks], axis=0).astype(BF16)
    total = jnp.dot(mix_hi[...], pieces, preferred_element_type=F32)
    total = total + jnp.dot(mix_lo[...], pieces, preferred_element_type=F32)
    half = total.shape[0] // CORES
    own[...] = total[:half]
    other[...] = total[half:].astype(BF16)


def expert_rows(rows, slices):
    contract = (((1,), (1,)), ((), ()))
    total = None
    for gate_w, up_w, down_w in slices:
        gate = lax.dot_general(rows, gate_w[...], contract, preferred_element_type=F32)
        upper = lax.dot_general(rows, up_w[...], contract, preferred_element_type=F32)
        hidden = (gate / (1.0 + jnp.exp(-gate)) * upper).astype(BF16)
        part = jnp.dot(hidden, down_w[...], preferred_element_type=F32)
        total = part if total is None else total + part
    return total.astype(BF16)


def ffn_kernel(gate_w, up_w, down_w, pack_a, pack_b, *refs, count):
    third = pack_a.shape[0] // 3
    slices = [(gate_w, up_w, down_w)] + [
        tuple(pack.at[pl.ds(i * third, third)] for i in range(3)) for pack in (pack_a, pack_b)
    ]
    sources, outs = refs[:count], refs[count : 2 * count]
    if count == 1:
        outs[0][...] = expert_rows(sources[0][...], slices)
        return
    taken, made = refs[2 * count :]
    for i in range(count):
        taken[i] = sources[i][...]

    @pl.loop(0, count)
    def _(i):
        made[i] = expert_rows(taken[i], slices)

    for i in range(count):
        outs[i][...] = made[i]


def chunks_of(chips):
    near = sorted(range(chips), key=lambda d: (min(d, chips - d), d))[: chips // 2]
    return [d for d in range(chips) if d not in near], near


def body(tokens, norm_gain, gate_weight, up_weight, down_weight, expert_ids, route_weight):
    tok_rows, width = tokens.shape
    n_tp = lax.axis_size("tp")
    n_ep = lax.axis_size("ep")
    chips = n_ep // CORES
    most = max(2, tok_rows * TOP_K * 5 // (4 * n_ep))
    slots = CORES * most
    ep = lax.axis_index("ep")
    tp = lax.axis_index("tp")
    place = jnp.stack([ep // CORES, ep % CORES]).astype(jnp.int32)

    def swap(values):
        return lax.ppermute(values, "ep", [(i, i ^ 1) for i in range(n_ep)])

    def over_chips(values, d):
        pairs = [(i, (i + CORES * d) % n_ep) for i in range(n_ep)]
        return lax.ppermute(values, "ep", pairs)

    def over_tp(values, step):
        return lax.ppermute(values, "tp", [(i, (i + step) % n_tp) for i in range(n_tp)])

    gate_t = gate_weight[0].T
    up_t = up_weight[0].T
    down = down_weight[0]
    part = gate_t.shape[0] // 2
    weights = (gate_t, up_t, down)
    pack_a = over_tp(jnp.concatenate([w[:part] for w in weights], axis=0), -1)
    pack_b = over_tp(jnp.concatenate([w[part:] for w in weights], axis=0), 1)

    tok_b = swap(tokens)
    own = lambda a: lax.dynamic_slice_in_dim(a.T, tp * tok_rows, tok_rows, 1)
    meta_a = jnp.concatenate(
        [own(expert_ids).astype(F32), own(route_weight), jnp.zeros((8 - 2 * TOP_K, tok_rows), F32)],
        axis=0,
    )
    meta_b = swap(meta_a)
    norm_a = pl.pallas_call(
        norm_kernel,
        in_specs=[VMEM] * 2,
        out_specs=VMEM,
        out_shape=jax.ShapeDtypeStruct(tokens.shape, BF16),
        compiler_params=PARAMS,
        name="norm_own",
    )(tokens, norm_gain[None])
    out_types = [jax.ShapeDtypeStruct((slots, width), BF16)] * chips
    out_types += [jax.ShapeDtypeStruct((CORES * tok_rows, chips * slots), BF16)] * 2
    *blocks, mix_hi, mix_lo = pl.pallas_call(
        functools.partial(dispatch_kernel, chips=chips, slots=slots),
        in_specs=[pl.BlockSpec(memory_space=pltpu.SMEM)] + [VMEM] * 5,
        out_specs=[VMEM] * (chips + 2),
        out_shape=out_types,
        scratch_shapes=[pltpu.VMEM((CORES * tok_rows, width), BF16)],
        compiler_params=PARAMS,
        name="dispatch",
    )(place, norm_a, tok_b, norm_gain[None], meta_a, meta_b)

    def ffn(*sources):
        n = len(sources)
        held = [pltpu.VMEM((n, *sources[0].shape), BF16)] * 2 if n > 1 else []
        return pl.pallas_call(
            functools.partial(ffn_kernel, count=n),
            in_specs=[VMEM] * (5 + n),
            out_specs=[VMEM] * n,
            out_shape=[jax.ShapeDtypeStruct(s.shape, BF16) for s in sources],
            scratch_shapes=held,
            compiler_params=PARAMS,
            name="ffn",
        )(gate_t, up_t, down, pack_a, pack_b, *sources)

    def add(got, part):
        return (got.astype(F32) + part.astype(F32)).astype(BF16)

    half = n_tp // (2 * HOP)
    groups = chunks_of(chips)
    chunks = [
        jnp.concatenate([over_chips(blocks[d], d) if d else blocks[d] for d in group], axis=0)
        for group in groups
    ]
    mine = ffn(*chunks)
    returned = [None] * chips
    for c, (group, way) in enumerate(zip(groups, (HOP, -HOP))):
        fore, back = [chunks[c]], [chunks[c]]
        for s in range(1, half + 1):
            fore.append(over_tp(fore[-1], way))
            if s < half:
                back.append(over_tp(back[-1], -way))
        parts = [None] + [ffn(fore[s], back[s]) for s in range(1, half)]
        (total_fore,) = ffn(fore[half])
        total_back = parts[half - 1][1]
        for h in range(1, half + 1):
            got = over_tp(total_fore, -way)
            total_fore = add(got, parts[half - h][0]) if h < half else got
        for h in range(1, half):
            got = over_tp(total_back, way)
            total_back = add(got, parts[half - 1 - h][1]) if h < half - 1 else got
        pieces = (
            mine[c].astype(F32) + total_fore.astype(F32) + total_back.astype(F32)
        ).astype(BF16)
        for j, d in enumerate(group):
            piece = pieces[j * slots : (j + 1) * slots]
            returned[d] = over_chips(piece, -d) if d else piece

    kept, other = pl.pallas_call(
        combine_kernel,
        in_specs=[VMEM] * (2 + chips),
        out_specs=[VMEM] * 2,
        out_shape=[
            jax.ShapeDtypeStruct((tok_rows, width), F32),
            jax.ShapeDtypeStruct((tok_rows, width), BF16),
        ],
        compiler_params=PARAMS,
        name="combine",
    )(mix_hi, mix_lo, *returned)
    return (kept + swap(other).astype(F32)).astype(BF16)


def solution(mesh):
    placed = (
        P(("grp", "ep", "tp"), None),
        P(),
        P("ep", None, "tp"),
        P("ep", None, "tp"),
        P("ep", "tp", None),
        P(("grp", "ep"), None),
        P(("grp", "ep"), None),
    )
    return jax.shard_map(
        body, mesh=mesh, in_specs=placed, out_specs=P(("grp", "ep", "tp"), None), check_vma=False
    )
```

```python
import functools

import jax
import jax.numpy as jnp
from jax import lax
from jax.experimental import pallas as pl
from jax.experimental.pallas import tpu as pltpu
from jax.sharding import PartitionSpec as P


TOP_K = 2
CORES = 2
F32 = jnp.float32
BF16 = jnp.bfloat16
VMEM = pl.BlockSpec(memory_space=pltpu.VMEM)
PARAMS = pltpu.CompilerParams(vmem_limit_bytes=24 * 1024 * 1024)


def norm_kernel(tok, gain, out):
    values = tok[...].astype(F32)
    scaled = values * lax.rsqrt(jnp.mean(values * values, axis=-1, keepdims=True) + 1e-06)
    out[...] = (scaled * gain[...]).astype(BF16)


def dispatch_kernel(place, norm_a, tok_b, gain, meta_a, meta_b, *refs, chips, slots):
    blocks, mix_hi, mix_lo, values = refs[:chips], refs[chips], refs[chips + 1], refs[chips + 2]
    chip, core = place[0], place[1]
    rows = norm_a.shape[0]
    both = CORES * rows
    total = chips * slots
    values[:rows] = norm_a[...]
    norm_kernel(tok_b, gain, values.at[rows:])
    meta = jnp.concatenate([meta_a[...].T, meta_b[...].T], axis=0)
    experts = meta[:, 0:TOP_K].astype(jnp.int32)
    distance = jnp.where(experts % CORES == core, (experts // CORES - chip + chips) % chips, -1)
    lane = lax.broadcasted_iota(jnp.int32, (both, 128), 1)
    hot = [lane == distance[:, k : k + 1] for k in range(TOP_K)]
    named = (hot[0] | hot[1]).astype(F32).astype(BF16)
    earlier = lax.broadcasted_iota(jnp.int32, (both, both), 1) < lax.broadcasted_iota(
        jnp.int32, (both, both), 0
    )
    rank = jnp.dot(earlier.astype(F32).astype(BF16), named, preferred_element_type=F32)
    row = lax.broadcasted_iota(jnp.int32, (both, total), 1)
    here = []
    for k in range(TOP_K):
        slot = jnp.sum(jnp.where(hot[k], rank, 0.0), axis=1, keepdims=True).astype(jnp.int32)
        at = jnp.where(distance[:, k : k + 1] < 0, -1, distance[:, k : k + 1] * slots + slot)
        here.append(row == at)
    send = (here[0] | here[1]).astype(F32).astype(BF16)
    packed = lax.dot_general(
        send, values[...], (((0,), (0,)), ((), ())), preferred_element_type=F32
    )
    for d in range(chips):
        blocks[d][...] = packed[d * slots : (d + 1) * slots].astype(BF16)
    mix = jnp.where(here[0], meta[:, TOP_K : TOP_K + 1], 0.0) + jnp.where(
        here[1], meta[:, TOP_K + 1 : TOP_K + 2], 0.0
    )
    high = mix.astype(BF16)
    mix_hi[...] = high
    mix_lo[...] = (mix - high.astype(F32)).astype(BF16)


def combine_kernel(mix_hi, mix_lo, *refs):
    blocks, own, other = refs[:-2], refs[-2], refs[-1]
    pieces = jnp.concatenate([b[...].astype(F32) for b in blocks], axis=0).astype(BF16)
    total = jnp.dot(mix_hi[...], pieces, preferred_element_type=F32)
    total = total + jnp.dot(mix_lo[...], pieces, preferred_element_type=F32)
    half = total.shape[0] // CORES
    own[...] = total[:half]
    other[...] = total[half:].astype(BF16)


def sum_kernel(mine, fore, back, *outs):
    total = mine[...].astype(F32) + fore[...].astype(F32) + back[...].astype(F32)
    rows = outs[0].shape[0]
    for j, out in enumerate(outs):
        out[...] = total[j * rows : (j + 1) * rows].astype(BF16)


def expert_rows(rows, gate_w, up_w, down_w):
    contract = (((1,), (1,)), ((), ()))
    gate = lax.dot_general(rows, gate_w[...], contract, preferred_element_type=F32)
    upper = lax.dot_general(rows, up_w[...], contract, preferred_element_type=F32)
    hidden = (gate / (1.0 + jnp.exp(-gate)) * upper).astype(BF16)
    return jnp.dot(hidden, down_w[...], preferred_element_type=F32).astype(BF16)


def ffn_kernel(gate_w, up_w, down_w, *refs, count):
    sources, outs = refs[:count], refs[count : 2 * count]
    if count == 1:
        outs[0][...] = expert_rows(sources[0][...], gate_w, up_w, down_w)
        return
    taken, made = refs[2 * count :]
    rows = taken.shape[1]
    tile = rows // 5 if rows % 80 == 0 else rows

    @pl.loop(0, rows // tile)
    def _(j):
        at = pl.ds(pl.multiple_of(j * tile, tile), tile)
        for i in range(count):
            taken[i, at] = sources[i][at]

    @pl.loop(0, count)
    def _(i):
        made[i] = expert_rows(taken[i], gate_w, up_w, down_w)

    @pl.loop(0, rows // tile)
    def _(j):
        at = pl.ds(pl.multiple_of(j * tile, tile), tile)
        for i in range(count):
            outs[i][at] = made[i, at]


def chunks_of(chips):
    near = sorted(range(chips), key=lambda d: (min(d, chips - d), d))[: chips // 2]
    return [d for d in range(chips) if d not in near], near


def body(tokens, norm_gain, gate_weight, up_weight, down_weight, expert_ids, route_weight):
    tok_rows, width = tokens.shape
    n_tp = lax.axis_size("tp")
    n_ep = lax.axis_size("ep")
    chips = n_ep // CORES
    most = max(2, tok_rows * TOP_K * 5 // (4 * n_ep))
    slots = CORES * most
    ep = lax.axis_index("ep")
    tp = lax.axis_index("tp")
    place = jnp.stack([ep // CORES, ep % CORES]).astype(jnp.int32)

    def swap(values):
        return lax.ppermute(values, "ep", [(i, i ^ 1) for i in range(n_ep)])

    def over_chips(values, d):
        pairs = [(i, (i + CORES * d) % n_ep) for i in range(n_ep)]
        return lax.ppermute(values, "ep", pairs)

    def over_tp(values, step):
        return lax.ppermute(values, "tp", [(i, (i + step) % n_tp) for i in range(n_tp)])

    gate_t = gate_weight[0].T
    up_t = up_weight[0].T
    down = down_weight[0]
    tok_b = swap(tokens)
    own = lambda a: lax.dynamic_slice_in_dim(a.T, tp * tok_rows, tok_rows, 1)
    meta_a = jnp.concatenate(
        [own(expert_ids).astype(F32), own(route_weight), jnp.zeros((8 - 2 * TOP_K, tok_rows), F32)],
        axis=0,
    )
    meta_b = swap(meta_a)
    norm_a = pl.pallas_call(
        norm_kernel,
        in_specs=[VMEM] * 2,
        out_specs=VMEM,
        out_shape=jax.ShapeDtypeStruct(tokens.shape, BF16),
        compiler_params=PARAMS,
        name="norm_own",
    )(tokens, norm_gain[None])
    out_types = [jax.ShapeDtypeStruct((slots, width), BF16)] * chips
    out_types += [jax.ShapeDtypeStruct((CORES * tok_rows, chips * slots), BF16)] * 2
    *blocks, mix_hi, mix_lo = pl.pallas_call(
        functools.partial(dispatch_kernel, chips=chips, slots=slots),
        in_specs=[pl.BlockSpec(memory_space=pltpu.SMEM)] + [VMEM] * 5,
        out_specs=[VMEM] * (chips + 2),
        out_shape=out_types,
        scratch_shapes=[pltpu.VMEM((CORES * tok_rows, width), BF16)],
        compiler_params=PARAMS,
        name="dispatch",
    )(place, norm_a, tok_b, norm_gain[None], meta_a, meta_b)

    def ffn(*sources):
        n = len(sources)
        held = [pltpu.VMEM((n, *sources[0].shape), BF16)] * 2 if n > 1 else []
        return pl.pallas_call(
            functools.partial(ffn_kernel, count=n),
            in_specs=[VMEM] * (3 + n),
            out_specs=[VMEM] * n,
            out_shape=[jax.ShapeDtypeStruct(s.shape, BF16) for s in sources],
            scratch_shapes=held,
            compiler_params=PARAMS,
            name="ffn",
        )(gate_t, up_t, down, *sources)

    def add(got, part):
        return (got.astype(F32) + part.astype(F32)).astype(BF16)

    half = n_tp // 2
    groups = chunks_of(chips)
    ways = (1, -1)
    chunks = [
        jnp.concatenate([over_chips(blocks[d], d) if d else blocks[d] for d in group], axis=0)
        for group in groups
    ]
    fore, back = [[chunk] for chunk in chunks], [[chunk] for chunk in chunks]
    for s in range(1, half + 1):
        for c, way in enumerate(ways):
            fore[c].append(over_tp(fore[c][-1], way))
            if s < half:
                back[c].append(over_tp(back[c][-1], -way))
    mine = ffn(*chunks)
    part_fore, part_back = [[None], [None]], [[None], [None]]
    for s in range(1, half - 1):
        made = ffn(fore[0][s], back[0][s], fore[1][s], back[1][s])
        for c in range(2):
            part_fore[c].append(made[2 * c])
            part_back[c].append(made[2 * c + 1])
    for c in range(2):
        made = ffn(fore[c][half - 1], back[c][half - 1])
        part_fore[c].append(made[0])
        part_back[c].append(made[1])
        part_fore[c] += ffn(fore[c][half])
    returned = [None] * chips
    for c, (group, way) in enumerate(zip(groups, ways)):
        total_fore, total_back = part_fore[c][half], part_back[c][half - 1]
        for h in range(1, half + 1):
            got = over_tp(total_fore, -way)
            total_fore = add(got, part_fore[c][half - h]) if h < half else got
        for h in range(1, half):
            got = over_tp(total_back, way)
            total_back = add(got, part_back[c][half - 1 - h]) if h < half - 1 else got
        pieces = pl.pallas_call(
            sum_kernel,
            in_specs=[VMEM] * 3,
            out_specs=[VMEM] * len(group),
            out_shape=[jax.ShapeDtypeStruct((slots, width), BF16)] * len(group),
            compiler_params=PARAMS,
            name="sum_blocks",
        )(mine[c], total_fore, total_back)
        for d, piece in zip(group, pieces):
            returned[d] = over_chips(piece, -d) if d else piece

    kept, other = pl.pallas_call(
        combine_kernel,
        in_specs=[VMEM] * (2 + chips),
        out_specs=[VMEM] * 2,
        out_shape=[
            jax.ShapeDtypeStruct((tok_rows, width), F32),
            jax.ShapeDtypeStruct((tok_rows, width), BF16),
        ],
        compiler_params=PARAMS,
        name="combine",
    )(mix_hi, mix_lo, *returned)
    return (kept + swap(other).astype(F32)).astype(BF16)


def solution(mesh):
    placed = (
        P(("grp", "ep", "tp"), None),
        P(),
        P("ep", None, "tp"),
        P("ep", None, "tp"),
        P("ep", "tp", None),
        P(("grp", "ep"), None),
        P(("grp", "ep"), None),
    )
    return jax.shard_map(
        body, mesh=mesh, in_specs=placed, out_specs=P(("grp", "ep", "tp"), None), check_vma=False
    )
```

```python
import functools

import jax
import jax.numpy as jnp
from jax import lax
from jax.experimental import pallas as pl
from jax.experimental.pallas import tpu as pltpu
from jax.sharding import PartitionSpec as P


TOP_K = 2
CORES = 2
HOP = 2
F32 = jnp.float32
BF16 = jnp.bfloat16
VMEM = pl.BlockSpec(memory_space=pltpu.VMEM)
PARAMS = pltpu.CompilerParams(vmem_limit_bytes=24 * 1024 * 1024)


def pack_kernel(gate_w, up_w, down_w, low, high, sems):
    part = low.shape[0] // 3
    copies = []
    for j, out in enumerate((low, high)):
        for i, weight in enumerate((gate_w, up_w, down_w)):
            source = weight.at[pl.ds(j * part, part)]
            target = out.at[pl.ds(i * part, part)]
            copies.append(pltpu.make_async_copy(source, target, sems.at[3 * j + i]))
    for copy in copies:
        copy.start()
    for copy in copies:
        copy.wait()


def norm_kernel(tok, gain, out):
    values = tok[...].astype(F32)
    scaled = values * lax.rsqrt(jnp.mean(values * values, axis=-1, keepdims=True) + 1e-06)
    out[...] = (scaled * gain[...]).astype(BF16)


def dispatch_kernel(place, norm_a, tok_b, gain, meta_a, meta_b, *refs, chips, slots):
    blocks, mix_hi, mix_lo, values = refs[:chips], refs[chips], refs[chips + 1], refs[chips + 2]
    chip, core = place[0], place[1]
    rows = norm_a.shape[0]
    both = CORES * rows
    total = chips * slots
    values[:rows] = norm_a[...]
    norm_kernel(tok_b, gain, values.at[rows:])
    meta = jnp.concatenate([meta_a[...].T, meta_b[...].T], axis=0)
    experts = meta[:, 0:TOP_K].astype(jnp.int32)
    distance = jnp.where(experts % CORES == core, (experts // CORES - chip + chips) % chips, -1)
    lane = lax.broadcasted_iota(jnp.int32, (both, 128), 1)
    hot = [lane == distance[:, k : k + 1] for k in range(TOP_K)]
    named = (hot[0] | hot[1]).astype(F32).astype(BF16)
    earlier = lax.broadcasted_iota(jnp.int32, (both, both), 1) < lax.broadcasted_iota(
        jnp.int32, (both, both), 0
    )
    rank = jnp.dot(earlier.astype(F32).astype(BF16), named, preferred_element_type=F32)
    row = lax.broadcasted_iota(jnp.int32, (both, total), 1)
    here = []
    for k in range(TOP_K):
        slot = jnp.sum(jnp.where(hot[k], rank, 0.0), axis=1, keepdims=True).astype(jnp.int32)
        at = jnp.where(distance[:, k : k + 1] < 0, -1, distance[:, k : k + 1] * slots + slot)
        here.append(row == at)
    send = (here[0] | here[1]).astype(F32).astype(BF16)
    packed = lax.dot_general(
        send, values[...], (((0,), (0,)), ((), ())), preferred_element_type=F32
    )
    for d in range(chips):
        blocks[d][...] = packed[d * slots : (d + 1) * slots].astype(BF16)
    mix = jnp.where(here[0], meta[:, TOP_K : TOP_K + 1], 0.0) + jnp.where(
        here[1], meta[:, TOP_K + 1 : TOP_K + 2], 0.0
    )
    high = mix.astype(BF16)
    mix_hi[...] = high
    mix_lo[...] = (mix - high.astype(F32)).astype(BF16)


def combine_kernel(mix_hi, mix_lo, *refs):
    blocks, own, other = refs[:-2], refs[-2], refs[-1]
    pieces = jnp.concatenate([b[...].astype(F32) for b in blocks], axis=0).astype(BF16)
    total = jnp.dot(mix_hi[...], pieces, preferred_element_type=F32)
    total = total + jnp.dot(mix_lo[...], pieces, preferred_element_type=F32)
    half = total.shape[0] // CORES
    own[...] = total[:half]
    other[...] = total[half:].astype(BF16)


def sum_kernel(mine, fore, back, *outs):
    total = mine[...].astype(F32) + fore[...].astype(F32) + back[...].astype(F32)
    rows = outs[0].shape[0]
    for j, out in enumerate(outs):
        out[...] = total[j * rows : (j + 1) * rows].astype(BF16)


def expert_rows(rows, slices):
    contract = (((1,), (1,)), ((), ()))
    total = None
    for gate_w, up_w, down_w in slices:
        gate = lax.dot_general(rows, gate_w[...], contract, preferred_element_type=F32)
        upper = lax.dot_general(rows, up_w[...], contract, preferred_element_type=F32)
        hidden = (gate / (1.0 + jnp.exp(-gate)) * upper).astype(BF16)
        part = jnp.dot(hidden, down_w[...], preferred_element_type=F32)
        total = part if total is None else total + part
    return total.astype(BF16)


def ffn_kernel(gate_w, up_w, down_w, pack_a, pack_b, *refs, count):
    third = pack_a.shape[0] // 3
    slices = [(gate_w, up_w, down_w)] + [
        tuple(pack.at[pl.ds(i * third, third)] for i in range(3)) for pack in (pack_a, pack_b)
    ]
    sources, outs = refs[:count], refs[count : 2 * count]
    if count == 1:
        outs[0][...] = expert_rows(sources[0][...], slices)
        return
    taken, made = refs[2 * count :]
    for i in range(count):
        taken[i] = sources[i][...]

    @pl.loop(0, count)
    def _(i):
        made[i] = expert_rows(taken[i], slices)

    for i in range(count):
        outs[i][...] = made[i]


def chunks_of(chips):
    near = sorted(range(chips), key=lambda d: (min(d, chips - d), d))[: chips // 2]
    return [d for d in range(chips) if d not in near], near


def body(tokens, norm_gain, gate_weight, up_weight, down_weight, expert_ids, route_weight):
    tok_rows, width = tokens.shape
    n_tp = lax.axis_size("tp")
    n_ep = lax.axis_size("ep")
    chips = n_ep // CORES
    most = max(2, tok_rows * TOP_K * 5 // (4 * n_ep))
    slots = CORES * most
    ep = lax.axis_index("ep")
    tp = lax.axis_index("tp")
    place = jnp.stack([ep // CORES, ep % CORES]).astype(jnp.int32)

    def swap(values):
        return lax.ppermute(values, "ep", [(i, i ^ 1) for i in range(n_ep)])

    def over_chips(values, d):
        pairs = [(i, (i + CORES * d) % n_ep) for i in range(n_ep)]
        return lax.ppermute(values, "ep", pairs)

    def over_tp(values, step):
        return lax.ppermute(values, "tp", [(i, (i + step) % n_tp) for i in range(n_tp)])

    def mirrored(values, step):
        pairs = [(i, (i + (step if i % HOP else -step)) % n_tp) for i in range(n_tp)]
        return lax.ppermute(values, "tp", pairs)

    gate_t = gate_weight[0].T
    up_t = up_weight[0].T
    down = down_weight[0]
    part = gate_t.shape[0] // 2
    low, high = pl.pallas_call(
        pack_kernel,
        in_specs=[pl.BlockSpec(memory_space=pltpu.HBM)] * 3,
        out_specs=[VMEM] * 2,
        out_shape=[jax.ShapeDtypeStruct((3 * part, width), BF16)] * 2,
        scratch_shapes=[pltpu.SemaphoreType.DMA((6,))],
        compiler_params=PARAMS,
        name="pack",
    )(gate_t, up_t, down)
    pack_a, pack_b = over_tp(low, -1), over_tp(high, 1)

    tok_b = swap(tokens)
    own = lambda a: lax.dynamic_slice_in_dim(a.T, tp * tok_rows, tok_rows, 1)
    meta_a = jnp.concatenate(
        [own(expert_ids).astype(F32), own(route_weight), jnp.zeros((8 - 2 * TOP_K, tok_rows), F32)],
        axis=0,
    )
    meta_b = swap(meta_a)
    norm_a = pl.pallas_call(
        norm_kernel,
        in_specs=[VMEM] * 2,
        out_specs=VMEM,
        out_shape=jax.ShapeDtypeStruct(tokens.shape, BF16),
        compiler_params=PARAMS,
        name="norm_own",
    )(tokens, norm_gain[None])
    out_types = [jax.ShapeDtypeStruct((slots, width), BF16)] * chips
    out_types += [jax.ShapeDtypeStruct((CORES * tok_rows, chips * slots), BF16)] * 2
    *blocks, mix_hi, mix_lo = pl.pallas_call(
        functools.partial(dispatch_kernel, chips=chips, slots=slots),
        in_specs=[pl.BlockSpec(memory_space=pltpu.SMEM)] + [VMEM] * 5,
        out_specs=[VMEM] * (chips + 2),
        out_shape=out_types,
        scratch_shapes=[pltpu.VMEM((CORES * tok_rows, width), BF16)],
        compiler_params=PARAMS,
        name="dispatch",
    )(place, norm_a, tok_b, norm_gain[None], meta_a, meta_b)

    def ffn(*sources):
        n = len(sources)
        held = [pltpu.VMEM((n, *sources[0].shape), BF16)] * 2 if n > 1 else []
        return pl.pallas_call(
            functools.partial(ffn_kernel, count=n),
            in_specs=[VMEM] * (5 + n),
            out_specs=[VMEM] * n,
            out_shape=[jax.ShapeDtypeStruct(s.shape, BF16) for s in sources],
            scratch_shapes=held,
            compiler_params=PARAMS,
            name="ffn",
        )(gate_t, up_t, down, pack_a, pack_b, *sources)

    def add(got, part):
        return (got.astype(F32) + part.astype(F32)).astype(BF16)

    half = n_tp // (2 * HOP)
    groups = chunks_of(chips)
    chunks = [
        jnp.concatenate([over_chips(blocks[d], d) if d else blocks[d] for d in group], axis=0)
        for group in groups
    ]
    mine = ffn(*chunks)
    returned = [None] * chips
    for c, (group, way) in enumerate(zip(groups, (HOP, -HOP))):
        fore, back = [chunks[c]], [chunks[c]]
        for s in range(1, half + 1):
            fore.append(mirrored(fore[-1], way))
            if s < half:
                back.append(mirrored(back[-1], -way))
        parts = [None] + [ffn(fore[s], back[s]) for s in range(1, half)]
        (total_fore,) = ffn(fore[half])
        total_back = parts[half - 1][1]
        for h in range(1, half + 1):
            got = mirrored(total_fore, -way)
            total_fore = add(got, parts[half - h][0]) if h < half else got
        for h in range(1, half):
            got = mirrored(total_back, way)
            total_back = add(got, parts[half - 1 - h][1]) if h < half - 1 else got
        pieces = pl.pallas_call(
            sum_kernel,
            in_specs=[VMEM] * 3,
            out_specs=[VMEM] * len(group),
            out_shape=[jax.ShapeDtypeStruct((slots, width), BF16)] * len(group),
            compiler_params=PARAMS,
            name="sum_blocks",
        )(mine[c], total_fore, total_back)
        for d, piece in zip(group, pieces):
            returned[d] = over_chips(piece, -d) if d else piece

    kept, other = pl.pallas_call(
        combine_kernel,
        in_specs=[VMEM] * (2 + chips),
        out_specs=[VMEM] * 2,
        out_shape=[
            jax.ShapeDtypeStruct((tok_rows, width), F32),
            jax.ShapeDtypeStruct((tok_rows, width), BF16),
        ],
        compiler_params=PARAMS,
        name="combine",
    )(mix_hi, mix_lo, *returned)
    return (kept + swap(other).astype(F32)).astype(BF16)


def solution(mesh):
    placed = (
        P(("grp", "ep", "tp"), None),
        P(),
        P("ep", None, "tp"),
        P("ep", None, "tp"),
        P("ep", "tp", None),
        P(("grp", "ep"), None),
        P(("grp", "ep"), None),
    )
    return jax.shard_map(
        body, mesh=mesh, in_specs=placed, out_specs=P(("grp", "ep", "tp"), None), check_vma=False
    )
```
